32 devices in a mesh: dp: 4 (over y, x), kv: 4 (over z), tp: 2 (over core).
Axes of the slice: x: 2, y: 2, z: 4, core: 2. Of those that a mesh axis runs over, the one named last changes fastest.
Arguments:
- tokens: bfloat16 [16, 4096], P('dp', ('kv', 'tp')), may hold values from -75 to 75, as said below
- attn_gain: bfloat16 [4096], P('kv'), may hold values from 0.099609375 to 1.8984375
- w_query: bfloat16 [4096, 2048], P('kv', 'tp'), may hold values from -0.09375 to 0.09375
- w_key: bfloat16 [4096, 256], P('kv', 'tp'), may hold values from -0.75 to 0.75
- w_value: bfloat16 [4096, 256], P('kv', 'tp'), may hold values from -0.09375 to 0.09375
- key_cache: bfloat16 [16, 8192, 2, 128], P('dp', 'kv', 'tp'), may hold values from -700 to 700
- value_cache: bfloat16 [16, 8192, 2, 128], P('dp', 'kv', 'tp'), may hold values from -6 to 6
- lam: float32 [16], P('tp'), may hold values from 0.3 to 0.8
- head_gain: bfloat16 [128], replicated, may hold values from 0.099609375 to 1.8984375
- w_out: bfloat16 [2048, 4096], P('tp', 'kv'), may hold values from -0.125 to 0.125
- ffn_gain: bfloat16 [4096], replicated, may hold values from 0.099609375 to 1.8984375
- w_up: bfloat16 [4096, 16384], P(None, ('dp', 'kv', 'tp')), may hold values from -0.09375 to 0.09375
- w_down: bfloat16 [16384, 4096], P(('dp', 'kv', 'tp')), may hold values from -0.09375 to 0.09375
Outputs:
- updated: bfloat16 [16, 4096], P('dp', ('kv', 'tp'))
The draws below stay inside these ranges and needn't reach their ends.
Inputs may be any that keep to these rules, and one draw needn't show every extreme that they name: `tokens`: column scales differ across the width.
All inputs are finite; a program needn't handle non-finite values.
Results may differ from the reference program's by a relative error of at most 0.017.
Values may be sent and summed in bfloat16 or wider, within the bound.
No kernel may reach another device: no remote copies, remote signals or barrier semaphores. Data moves between devices by JAX's collectives and lax.ppermute only.
A program may use at most 64 MiB of HBM per device.

```python
import math
import jax
import jax.numpy as jnp
from jax import lax

D = 4096
HEADS = 16
KV_HEADS = 2
HD = 64
VD = 128
FF = 16384
SEQ_DEV = 4
POS_DEV = 2048
BATCH = 16
LENGTH = 8192
N_DP = 4
N_KV = 4
N_TP = 2


def draw_tokens(key, part):
    batch = SEQ_DEV * N_DP
    first, second = jax.random.split(key, 2)
    rough = jax.random.uniform(second, (D,), jnp.float32, 0.7, 1.4)
    column = jnp.exp(jnp.linspace(0.0, math.log(3.5), D)).astype(jnp.float32)
    base = jnp.clip(jax.random.normal(first, (batch, D), jnp.float32), -5.0, 5.0)
    return (base * column * rough).astype(jnp.bfloat16)


def draw_key_cache(key, part):
    batch = SEQ_DEV * N_DP
    length = POS_DEV * N_KV
    wide = 2 * HD
    keys = jax.random.split(key, 1)
    base = jnp.clip(jax.random.normal(keys[0], (batch, length, KV_HEADS, wide), jnp.float32), -6.0, 6.0) * 1.75
    return base.astype(jnp.bfloat16)


def with_spikes(values, own_key, source, target, shards_of, factor):
    def block_of(axis_at):
        return (jnp.arange(values.shape[axis_at]) // (values.shape[axis_at] // shards_of)).reshape((-1,) + (1,) * (values.ndim - 1 - axis_at))

    first = jax.random.permutation(own_key, shards_of)[block_of(target)]
    second = (block_of(target) + shards_of // 2) % shards_of
    return jnp.where((block_of(source) == first) | (block_of(source) == second), factor * values, values)


def shard_levels(stream_key, dims, shards, smallest, largest):
    factor_of, own = 1.0, jax.random.fold_in(stream_key, 6)
    for dim, blocks in shards:
        heights = jnp.exp(jax.random.uniform(jax.random.fold_in(own, dim), (blocks,), jnp.float32, smallest / len(shards), largest / len(shards)))
        factor_of = factor_of * jnp.repeat(heights, dims[dim] // blocks).reshape([-1 if axis == dim else 1 for axis in range(len(dims))])
    return factor_of


def gaussian(stream_key, extent, spread, most, shards=(), held_as=jnp.bfloat16):
    values = spread * jax.random.normal(stream_key, extent, jnp.float32)
    if shards:
        values = values * shard_levels(stream_key, extent, shards, -0.22, 0.18)
    return jnp.clip(values, -most, most).astype(held_as)


def bell_draw_with(key, dims, deviation, most, pieces, heavy, kind=jnp.bfloat16):
    entries = deviation * jax.random.normal(key, dims, jnp.float32)
    if pieces:
        entries = entries * shard_levels(key, dims, pieces, -0.22, 0.18)
    return jnp.clip(with_spikes(entries, jax.random.fold_in(key, 3), *heavy), -most, most).astype(kind)


def setup_inputs(seed: int = 0) -> dict:
    key_list = jax.random.split(jax.random.key(seed), 14)
    tokens = draw_tokens(jax.random.fold_in(key_list[13], 71), 0)
    attn_gain = jnp.clip(1.0 + 0.18 * jax.random.normal(key_list[1], (D,), jnp.float32), 0.099609375, 1.8984375).astype(jnp.bfloat16)
    w_query = gaussian(key_list[2], (D, HEADS * 2 * HD), D ** -0.5, 0.09375, ((0, 4), (1, 2)))
    w_key = gaussian(key_list[3], (D, KV_HEADS * 2 * HD), (D // 64) ** -0.5, 0.75, ((0, 4), (1, 2)))
    w_value = gaussian(key_list[4], (D, KV_HEADS * VD), D ** -0.5, 0.09375, ((0, 4), (1, 2)))
    key_cache = draw_key_cache(jax.random.fold_in(key_list[13], 71), 0)
    value_cache = gaussian(key_list[6], (BATCH, LENGTH, KV_HEADS, VD), 1.0, 6.0, ((0, 4), (1, 4), (2, 2)))
    lam = jnp.clip(0.3 + 0.5 * jax.random.uniform(key_list[7], (HEADS,), jnp.float32) ** shard_levels(key_list[7], (HEADS,), ((0, 2),), -0.2, 0.2), 0.3, 0.8)
    head_gain = jnp.clip(1.0 + 0.18 * jax.random.normal(key_list[8], (VD,), jnp.float32), 0.099609375, 1.8984375).astype(jnp.bfloat16)
    w_out = gaussian(key_list[9], (HEADS * VD, D), (HEADS * VD) ** -0.5, 0.125, ((0, 2), (1, 4)))
    ffn_gain = jnp.clip(1.0 + 0.18 * jax.random.normal(key_list[10], (D,), jnp.float32), 0.099609375, 1.8984375).astype(jnp.bfloat16)
    w_up = gaussian(key_list[11], (D, FF), D ** -0.5, 0.09375, ((1, 32),))
    w_down = bell_draw_with(key_list[12], (FF, D), FF ** -0.5, 0.09375, ((0, 32),), (0, 1, 32, 2.75))
    return {"tokens": tokens, "attn_gain": attn_gain, "w_query": w_query, "w_key": w_key, "w_value": w_value, "key_cache": key_cache, "value_cache": value_cache, "lam": lam, "head_gain": head_gain, "w_out": w_out, "ffn_gain": ffn_gain, "w_up": w_up, "w_down": w_down}


EPS = 1e-06
THETA = 500000.0
OUT_SCALE = 0.8

def settle(value):
    return lax.optimization_barrier(value.astype(jnp.bfloat16)).astype(jnp.float32)

def rotate(value, position):
    half = value.shape[-1] // 2
    inverse = THETA ** (-jnp.arange(half, dtype=jnp.float32) * 2.0 / value.shape[-1])
    angle = position * inverse
    cosine = jnp.cos(angle)
    sine = jnp.sin(angle)
    first = value[..., :half]
    second = value[..., half:]
    return jnp.concatenate([first * cosine - second * sine, second * cosine + first * sine], axis=-1)

def reference(tokens, attn_gain, w_query, w_key, w_value, key_cache, value_cache, lam, head_gain, w_out, ffn_gain, w_up, w_down):
    f32 = jnp.float32
    bf = jnp.bfloat16
    batch = tokens.shape[0]
    length = key_cache.shape[1]
    group = HEADS // KV_HEADS
    scale = HD ** (-0.5)
    xf = tokens.astype(f32)
    inv_rms = lax.rsqrt(lax.optimization_barrier(jnp.mean(xf * xf, axis=-1, keepdims=True)) + EPS)
    scaled = (xf * attn_gain.astype(f32)).astype(bf)
    q_raw = jnp.dot(scaled, w_query, preferred_element_type=f32) * inv_rms
    k_raw = jnp.dot(scaled, w_key, preferred_element_type=f32) * inv_rms
    v_raw = jnp.dot(scaled, w_value, preferred_element_type=f32) * inv_rms
    position = jnp.asarray(length, f32)
    query = settle(rotate(q_raw.reshape(batch, KV_HEADS, group, 2, HD), position))
    new_key = settle(rotate(k_raw.reshape(batch, KV_HEADS, 2, HD), position))
    new_value = settle(v_raw.reshape(batch, KV_HEADS, VD))
    own_score = jnp.einsum('bkgmd,bkmd->bkgm', query, new_key) * scale

    def one_sequence(items):
        query_b, keys_b, values_b, own_b, newval_b = items
        keys_f = keys_b.reshape(length, KV_HEADS, 2, HD).astype(f32)
        scores = jnp.einsum('kgmd,lkmd->kgml', query_b, keys_f) * scale
        top = jnp.maximum(lax.optimization_barrier(jnp.max(scores, axis=-1)), own_b)
        expo = jnp.exp(scores - top[..., None])
        own_w = jnp.exp(own_b - top)
        den = lax.optimization_barrier(jnp.sum(expo, axis=-1)) + own_w
        num = jnp.einsum('kgml,lkv->kgmv', settle(expo), values_b.astype(f32))
        num = num + settle(own_w)[..., None] * newval_b[:, None, None, :]
        return (num, den)
    num, den = lax.map(one_sequence, (query, key_cache, value_cache, own_score, new_value))
    lam_h = lam.astype(f32).reshape(KV_HEADS, group)
    mix = num[..., 0, :] / den[..., 0, None] - lam_h[None, :, :, None] * num[..., 1, :] / den[..., 1, None]
    normed = mix * lax.rsqrt(lax.optimization_barrier(jnp.mean(mix * mix, axis=-1, keepdims=True)) + EPS) * head_gain.astype(f32) * OUT_SCALE
    attended = normed.astype(bf).reshape(batch, N_TP, HEADS * VD // N_TP).astype(f32)
    out_parts = jnp.einsum('btk,tkd->btd', attended, w_out.reshape(N_TP, HEADS * VD // N_TP, D).astype(f32))
    branch = lax.optimization_barrier(jnp.sum(settle(out_parts), axis=1))
    hidden = lax.optimization_barrier((xf + branch).astype(bf))
    hf = hidden.astype(f32)
    inv_two = lax.rsqrt(lax.optimization_barrier(jnp.mean(hf * hf, axis=-1, keepdims=True)) + EPS)
    normed_two = (hf * inv_two * ffn_gain.astype(f32)).astype(bf)
    upward = jnp.dot(normed_two, w_up, preferred_element_type=f32)
    act = jnp.square(jax.nn.relu(upward)).astype(bf)
    down = jnp.dot(act, w_down, preferred_element_type=f32)
    return (hf + down).astype(bf)
```

```python
import jax
import jax.numpy as jnp
from jax import lax
from jax.sharding import PartitionSpec as P

D = 4096
HD = 64
VD = 128


EPS = 1e-06
THETA = 500000.0
OUT_SCALE = 0.8


def everyones(value, axis):
    count = lax.axis_size(axis)
    if count > 8:
        copies = jnp.broadcast_to(value[None], (count,) + value.shape)
        got = lax.all_to_all(copies, axis, 0, 0, tiled=True)
        return [got[k] for k in range(count)]
    return [value] + [
        lax.ppermute(value, axis, [(i, (i + step) % count) for i in range(count)])
        for step in range(1, count)
    ]


def split3(value):
    bf = jnp.bfloat16
    f32 = jnp.float32
    high = lax.reduce_precision(value, 8, 7)
    rest = value - high
    middle = lax.reduce_precision(rest, 8, 7)
    low = lax.reduce_precision(rest - middle, 8, 7)
    return [part.astype(bf) for part in (high, middle, low)]


def join3(parts):
    f32 = jnp.float32
    high, middle, low = (part.astype(f32) for part in parts)
    return high + (middle + low)


def settle(value):
    return lax.reduce_precision(value, 8, 7)


def rotate(value, position):
    half = value.shape[-1] // 2
    inverse = THETA ** (-jnp.arange(half, dtype=jnp.float32) * 2.0 / value.shape[-1])
    angle = position * inverse
    cosine = jnp.cos(angle)
    sine = jnp.sin(angle)
    first = value[..., :half]
    second = value[..., half:]
    return jnp.concatenate(
        [first * cosine - second * sine, second * cosine + first * sine], axis=-1
    )


def local(
    tokens,
    attn_gain,
    w_query,
    w_key,
    w_value,
    key_cache,
    value_cache,
    lam,
    head_gain,
    w_out,
    ffn_gain,
    w_up,
    w_down,
):
    f32 = jnp.float32
    bf = jnp.bfloat16
    rows, width = tokens.shape
    kv_count = lax.axis_size("kv")
    tp_count = lax.axis_size("tp")
    dp_count = lax.axis_size("dp")
    me_tp = lax.axis_index("tp")
    positions = key_cache.shape[1]
    kv_local = key_cache.shape[2]
    heads_local = lam.shape[0]
    group = heads_local // kv_local
    scale = HD ** (-0.5)
    axes = ("dp", "kv", "tp")
    assert tp_count == 2
    swap = [(0, 1), (1, 0)]

    other = lax.ppermute(tokens, "tp", swap)
    slab = jnp.where(
        me_tp == 0,
        jnp.concatenate([tokens, other], axis=1),
        jnp.concatenate([other, tokens], axis=1),
    )
    slab_f = slab.astype(f32)
    scaled = (slab_f * attn_gain.astype(f32)).astype(bf)
    part_q = jnp.dot(scaled, w_query, preferred_element_type=f32)
    part_k = jnp.dot(scaled, w_key, preferred_element_type=f32)
    part_v = jnp.dot(scaled, w_value, preferred_element_type=f32)
    local_sq = jnp.sum(slab_f * slab_f, axis=-1, keepdims=True)
    packed = jnp.concatenate(
        [part_q, part_k, part_v, jnp.broadcast_to(local_sq, (rows, 128))], axis=1
    )
    total = sum(everyones(packed, "kv"))
    width_q = part_q.shape[1]
    width_k = part_k.shape[1]
    width_v = part_v.shape[1]
    total_q = total[:, :width_q]
    total_k = total[:, width_q : width_q + width_k]
    total_v = total[:, width_q + width_k : width_q + width_k + width_v]
    total_sq = total[:, width_q + width_k + width_v :][:, :1]
    inv_rms = lax.rsqrt(total_sq / D + EPS)
    position = jnp.asarray(positions * kv_count, f32)
    query = rotate((total_q * inv_rms).reshape(rows, kv_local, group, 2, HD), position).astype(bf)
    new_key = rotate((total_k * inv_rms).reshape(rows, kv_local, 2, HD), position).astype(bf)
    new_value = (total_v * inv_rms).astype(bf).reshape(rows, kv_local, VD)

    zero = jnp.zeros_like(query[..., 0, :])
    wide = jnp.stack(
        [
            jnp.concatenate([query[..., 0, :], zero], axis=-1),
            jnp.concatenate([zero, query[..., 1, :]], axis=-1),
        ],
        axis=3,
    )
    scores = (
        jnp.einsum("rkgmd,rpkd->rkgmp", wide, key_cache, preferred_element_type=f32) * scale
    )
    local_top = jnp.max(scores, axis=-1)
    expo = jnp.exp(scores - local_top[..., None])
    local_den = jnp.sum(expo, axis=-1)
    local_num = jnp.einsum(
        "rkgmp,rpkv->rkgmv", expo.astype(bf), value_cache, preferred_element_type=f32
    )
    parts = split3(local_top) + split3(local_den)
    stats = jnp.stack(parts, axis=0).reshape(len(parts), -1)
    flat_num = local_num.astype(bf).reshape(-1, VD)
    stats = stats.reshape(-1, VD)
    pad = -stats.shape[0] % 16
    message = jnp.concatenate([flat_num, jnp.pad(stats, ((0, pad), (0, 0)))], axis=0)
    tops = []
    dens = []
    nums = []
    for got in everyones(message, "kv"):
        nums.append(got[: flat_num.shape[0]].astype(f32).reshape(local_num.shape))
        held = got[flat_num.shape[0] :][: stats.shape[0]].reshape((len(parts),) + local_top.shape)
        tops.append(join3(held[:3]))
        dens.append(join3(held[3:]))
    own_score = jnp.einsum("rkgmd,rkmd->rkgm", query, new_key, preferred_element_type=f32) * scale
    final_top = own_score
    for top in tops:
        final_top = jnp.maximum(final_top, top)
    own_weight = jnp.exp(own_score - final_top)
    den = own_weight
    num = settle(own_weight)[..., None] * new_value.astype(f32)[:, :, None, None, :]
    for top, den_k, num_k in zip(tops, dens, nums):
        carried = jnp.exp(top - final_top)
        den = den + den_k * carried
        num = num + num_k * carried[..., None]
    lam_h = lam.reshape(kv_local, group)
    mix = (
        num[..., 0, :] / den[..., 0, None]
        - lam_h[None, :, :, None] * num[..., 1, :] / den[..., 1, None]
    )
    normed = (
        mix
        * lax.rsqrt(jnp.mean(mix * mix, axis=-1, keepdims=True) + EPS)
        * head_gain.astype(f32)
        * OUT_SCALE
    )
    attended = normed.astype(bf).reshape(rows, heads_local * VD)
    part_out = jnp.dot(attended, w_out, preferred_element_type=f32).astype(bf)
    low = part_out[:, :width]
    high = part_out[:, width:]
    mine = jnp.where(me_tp == 0, low, high)
    theirs = jnp.where(me_tp == 0, high, low)
    received = lax.ppermute(theirs, "tp", swap)
    branch = mine.astype(f32) + received.astype(f32)
    hidden = (tokens.astype(f32) + branch).astype(bf)
    devices = dp_count * kv_count * tp_count
    everyone = lax.all_to_all(
        jnp.broadcast_to(hidden[None], (devices,) + hidden.shape), axes, 0, 0, tiled=True
    )
    blocks = kv_count * tp_count
    grid = everyone.reshape(dp_count, blocks, rows, width).astype(f32)
    row_sq = jnp.sum(grid * grid, axis=(1, 3))
    inv_two = lax.rsqrt(row_sq / D + EPS)
    gains = ffn_gain.astype(f32).reshape(blocks, width)
    normed_two = (grid * inv_two[:, None, :, None] * gains[None, :, None, :]).astype(bf)
    upward = jnp.einsum(
        "acrd,cdf->arf",
        normed_two,
        w_up.reshape(blocks, width, w_up.shape[1]),
        preferred_element_type=f32,
    )
    act = jnp.square(jax.nn.relu(upward)).astype(bf)
    down = jnp.einsum(
        "arf,fcd->acrd",
        act,
        w_down.reshape(w_down.shape[0], blocks, width),
        preferred_element_type=f32,
    )
    term = down.astype(bf).reshape(devices, rows, width)
    terms = lax.all_to_all(term, axes, 0, 0, tiled=True)
    mixed = jnp.sum(terms.astype(f32), axis=0)
    return (hidden.astype(f32) + mixed).astype(bf)


def solution(mesh):
    in_specs = (
        P("dp", ("kv", "tp")),
        P("kv"),
        P("kv", "tp"),
        P("kv", "tp"),
        P("kv", "tp"),
        P("dp", "kv", "tp", None),
        P("dp", "kv", "tp", None),
        P("tp"),
        P(),
        P("tp", "kv"),
        P(),
        P(None, ("dp", "kv", "tp")),
        P(("dp", "kv", "tp"), None),
    )
    out_specs = P("dp", ("kv", "tp"))
    return jax.shard_map(local, mesh=mesh, in_specs=in_specs, out_specs=out_specs, check_vma=False)
```

```python
import functools
import numpy as np
import jax
import jax.numpy as jnp
from jax import lax
from jax.experimental import pallas as pl
from jax.experimental.pallas import tpu as pltpu
from jax.sharding import PartitionSpec as P

D = 4096
HD = 64
VD = 128
EPS = 1e-06
THETA = 500000.0
OUT_SCALE = 0.8
LANES = 128
FAR = -3e38

F32 = jnp.float32
BF = jnp.bfloat16
VMEM = pl.BlockSpec(memory_space=pltpu.VMEM)
SMEM = pl.BlockSpec(memory_space=pltpu.SMEM)
ANY = pl.BlockSpec(memory_space=pl.ANY)


def everyones(value, axis):
    count = lax.axis_size(axis)
    if count > 8:
        copies = jnp.broadcast_to(value[None], (count,) + value.shape)
        got = lax.all_to_all(copies, axis, 0, 0, tiled=True)
        return [got[k] for k in range(count)]
    got = [value]
    for step in reversed(range(1, count)):
        got.append(lax.ppermute(value, axis, [(i, i ^ step) for i in range(count)]))
    return got


def rounded(value):
    return value.astype(BF).astype(F32)


def flat_row(ref, first, count):
    return jnp.concatenate([ref[first + i : first + i + 1, :] for i in range(count)], axis=1)


def project_kernel(tokens, other, gain, w_query, w_key, w_value, out):
    first = lax.axis_index("tp") == 0
    own = tokens[...].astype(F32)
    their = other[...].astype(F32)
    slab = jnp.concatenate([jnp.where(first, own, their), jnp.where(first, their, own)], axis=1)
    gains = flat_row(gain[...].astype(F32), 0, gain.shape[0])
    scaled = (slab * gains).astype(BF)
    q = w_query.shape[1]
    k = q + w_key.shape[1]
    v = k + w_value.shape[1]
    out[:, :q] = jnp.dot(scaled, w_query[...], preferred_element_type=F32)
    out[:, q:k] = jnp.dot(scaled, w_key[...], preferred_element_type=F32)
    out[:, k:v] = jnp.dot(scaled, w_value[...], preferred_element_type=F32)
    square = jnp.sum(slab * slab, axis=1, keepdims=True)
    out[:, v:] = jnp.broadcast_to(square, (slab.shape[0], LANES))


def attend_kernel(heads, parts, table, keys, values, out):
    total = parts[0][...]
    for part in parts[1:]:
        total = total + part[...]
    rows = total.shape[0]
    width = total.shape[1] - LANES
    inverse = lax.rsqrt(total[:, width : width + 1] / D + EPS)
    total = total[:, :width] * inverse
    cosine = table[0:1, :]
    sine = table[1:2, :]
    lane = lax.broadcasted_iota(jnp.int32, (rows, LANES), 1)
    near = lax.rem(lane, HD) < HD // 2

    def rotate(piece):
        ahead = pltpu.roll(piece, LANES - HD // 2, 1)
        behind = pltpu.roll(piece, HD // 2, 1)
        return rounded(piece * cosine + jnp.where(near, ahead, behind) * sine)

    pieces = [total[:, h * LANES : (h + 1) * LANES] for h in range(heads + 2)]
    query = [rotate(piece) * (HD**-0.5) for piece in pieces[:heads]]
    new_key = rotate(pieces[heads])
    new_value = rounded(pieces[heads + 1])
    holds_new = lax.axis_index("kv") == 0
    lane_h = lax.broadcasted_iota(jnp.int32, (heads, LANES), 1)
    lane_s = lax.broadcasted_iota(jnp.int32, (2 * heads, LANES), 1)
    stats = jnp.zeros((2 * heads, LANES), F32)
    for r in range(rows):
        mine = jnp.concatenate([piece[r : r + 1, :] for piece in query], axis=0)
        wide = jnp.concatenate(
            [jnp.where(lane_h < HD, mine, 0.0), jnp.where(lane_h < HD, 0.0, mine)], axis=0
        )
        scores = lax.dot_general(
            wide.astype(BF), keys[r], (((1,), (1,)), ((), ())), preferred_element_type=F32
        )
        own = jnp.sum(wide * new_key[r : r + 1, :], axis=1, keepdims=True)
        own = jnp.where(holds_new, own, FAR)
        top = jnp.maximum(jnp.max(scores, axis=1, keepdims=True), own)
        weights = jnp.exp(scores - top)
        own_weight = jnp.exp(own - top)
        den = jnp.sum(weights, axis=1, keepdims=True) + own_weight
        num = jnp.dot(weights.astype(BF), values[r], preferred_element_type=F32)
        num = num + rounded(own_weight) * new_value[r : r + 1, :]
        out[2 * heads * r : 2 * heads * (r + 1), :] = num.astype(BF)
        for at, value in ((r, top), (rows + r, den)):
            high = rounded(value)
            middle = rounded(value - high)
            low = rounded(value - high - middle)
            for step, piece in enumerate((high, middle, low)):
                stats = jnp.where(lane_s == 2 * rows * step + at, piece, stats)
    out[2 * heads * rows :, :] = stats.astype(BF)


def merge_kernel(heads, rows, messages, lam, head_gain, w_out, mine, theirs):
    first = lax.axis_index("tp") == 0
    span = 2 * heads
    joined = []
    for message in messages:
        stats = message[span * rows :, :].astype(F32)
        middle = pltpu.roll(stats, LANES - 2 * rows, 1)
        low = pltpu.roll(stats, LANES - 4 * rows, 1)
        joined.append(stats + (middle + low))
    top = functools.reduce(jnp.maximum, joined)
    carried = [jnp.exp(part - top) for part in joined]
    den = sum(c * pltpu.roll(part, LANES - rows, 1) for c, part in zip(carried, joined))
    shares = [c / den for c in carried]
    sub = lax.broadcasted_iota(jnp.int32, (heads, LANES), 0)
    lams = jnp.zeros((heads, LANES), F32)
    for h in range(heads):
        lams = jnp.where(sub == h, lam[h], lams)
    gains = head_gain[...].astype(F32) * OUT_SCALE
    attended = []
    for r in range(rows):
        ratio = sum(
            share[:, r : r + 1] * message[span * r : span * (r + 1), :].astype(F32)
            for share, message in zip(shares, messages)
        )
        mix = ratio[:heads] - lams * ratio[heads:]
        spread = lax.rsqrt(jnp.mean(mix * mix, axis=1, keepdims=True) + EPS)
        attended.append(mix * spread * gains)
    wide = jnp.concatenate(
        [
            jnp.concatenate([part[h : h + 1, :] for part in attended], axis=0)
            for h in range(heads)
        ],
        axis=1,
    )
    branch = jnp.dot(wide.astype(BF), w_out[...], preferred_element_type=F32)
    half = branch.shape[1] // 2
    mine[...] = jnp.where(first, branch[:, :half], branch[:, half:]).astype(BF)
    theirs[...] = jnp.where(first, branch[:, half:], branch[:, :half]).astype(BF)


def hidden_kernel(tokens, mine, received, copies, hidden):
    branch = mine[...].astype(F32) + received[...].astype(F32)
    value = (tokens[...].astype(F32) + branch).astype(BF)
    hidden[...] = value
    for k in range(copies.shape[0]):
        copies[k] = value


def mixer_kernel(dps, everyone, gain, w_up, w_down, out):
    devices, rows, width = everyone.shape
    blocks = devices // dps
    grid = []
    square = jnp.zeros((dps * rows, 1), F32)
    for b in range(blocks):
        block = jnp.concatenate(
            [everyone[a * blocks + b].astype(F32) for a in range(dps)], axis=0
        )
        grid.append(block)
        square = square + jnp.sum(block * block, axis=1, keepdims=True)
    inverse = lax.rsqrt(square / D + EPS)
    per = width // LANES
    gains = gain[...].astype(F32)
    upward = jnp.zeros((dps * rows, w_up.shape[1]), F32)
    for b in range(blocks):
        normed = (grid[b] * inverse * flat_row(gains, b * per, per)).astype(BF)
        upward = upward + jnp.dot(
            normed, w_up[b * width : (b + 1) * width, :], preferred_element_type=F32
        )
    act = jnp.square(jnp.maximum(upward, 0.0)).astype(BF)
    for b in range(blocks):
        down = jnp.dot(
            act, w_down[:, b * width : (b + 1) * width], preferred_element_type=F32
        ).astype(BF)
        for a in range(dps):
            out[a * blocks + b] = down[a * rows : (a + 1) * rows, :]


def final_kernel(terms, hidden, out):
    total = terms[0].astype(F32)
    for k in range(1, terms.shape[0]):
        total = total + terms[k].astype(F32)
    out[...] = (hidden[...].astype(F32) + total).astype(BF)


def load_kernel(count, *refs):
    sources, held, sems = refs[:count], refs[count : 2 * count], refs[2 * count]
    copies = [
        pltpu.make_async_copy(source, target, sems.at[i])
        for i, (source, target) in enumerate(zip(sources, held))
    ]
    for copy in copies:
        copy.start()
    for copy in copies:
        copy.wait()


def loaded(*arrays):
    count = len(arrays)
    size = sum(array.size * array.dtype.itemsize for array in arrays)
    return pl.pallas_call(
        functools.partial(load_kernel, count),
        out_shape=[jax.ShapeDtypeStruct(array.shape, array.dtype) for array in arrays],
        in_specs=[pl.BlockSpec(memory_space=pltpu.HBM)] * count,
        out_specs=[VMEM] * count,
        scratch_shapes=[pltpu.SemaphoreType.DMA((count,))],
        compiler_params=pltpu.CompilerParams(vmem_limit_bytes=1 << 20),
        cost_estimate=pl.CostEstimate(flops=20 * size, bytes_accessed=size, transcendentals=0),
    )(*(pltpu.with_memory_space_constraint(array, pltpu.HBM) for array in arrays))


def tables(position):
    half = HD // 2
    angle = position * THETA ** (-np.arange(half, dtype=np.float64) * 2.0 / HD)
    cosine = np.tile(np.cos(angle), LANES // half)
    sine = np.tile(np.concatenate([-np.sin(angle), np.sin(angle)]), LANES // HD)
    rest = np.zeros((6, LANES))
    return jnp.asarray(np.concatenate([cosine[None], sine[None], rest]), F32)


def call(kernel, shapes, inputs, specs, mib):
    return pl.pallas_call(
        kernel,
        out_shape=shapes,
        in_specs=specs,
        out_specs=jax.tree.map(lambda _: VMEM, shapes),
        compiler_params=pltpu.CompilerParams(vmem_limit_bytes=mib << 20),
    )(*inputs)


def local(
    tokens,
    attn_gain,
    w_query,
    w_key,
    w_value,
    key_cache,
    value_cache,
    lam,
    head_gain,
    w_out,
    ffn_gain,
    w_up,
    w_down,
):
    rows, width = tokens.shape
    kv_count = lax.axis_size("kv")
    tp_count = lax.axis_size("tp")
    dp_count = lax.axis_size("dp")
    positions = key_cache.shape[1]
    heads = lam.shape[0]
    axes = ("dp", "kv", "tp")
    swap = [(0, 1), (1, 0)]
    assert tp_count == 2 and key_cache.shape[2] == 1 and 6 * rows <= LANES
    shape = jax.ShapeDtypeStruct

    other = lax.ppermute(tokens, "tp", swap)
    packed = w_query.shape[1] + w_key.shape[1] + w_value.shape[1] + LANES
    held, gain, query, key, value = loaded(
        tokens, attn_gain.reshape(-1, LANES), w_query, w_key, w_value
    )
    part = call(
        project_kernel,
        shape((rows, packed), F32),
        (held, other, gain, query, key, value),
        [VMEM] * 6,
        6,
    )
    parts = everyones(part, "kv")
    table, keys, values = loaded(
        tables(positions * kv_count),
        key_cache.reshape(rows, positions, 2 * HD),
        value_cache.reshape(rows, positions, VD),
    )
    count = len(parts)

    def attend(*refs):
        attend_kernel(heads, refs[:count], *refs[count:])

    message = call(
        attend,
        shape((2 * heads * (rows + 1), LANES), BF),
        (*parts, table, keys, values),
        [VMEM] * (count + 3),
        8,
    )
    messages = everyones(message, "kv")
    head_gain, w_out = loaded(head_gain.reshape(1, VD), w_out)

    def merge(*refs):
        merge_kernel(heads, rows, refs[:count], *refs[count:])

    mine, theirs = call(
        merge,
        (shape((rows, width), BF), shape((rows, width), BF)),
        (*messages, lam, head_gain, w_out),
        [VMEM] * count + [SMEM, VMEM, VMEM],
        5,
    )
    received = lax.ppermute(theirs, "tp", swap)
    devices = dp_count * kv_count * tp_count
    copies, hidden = call(
        hidden_kernel,
        (shape((devices, rows, width), BF), shape((rows, width), BF)),
        (held, mine, received),
        [VMEM] * 3,
        2,
    )
    everyone = lax.all_to_all(copies, axes, 0, 0, tiled=True)
    term = call(
        functools.partial(mixer_kernel, dp_count),
        shape((devices, rows, width), BF),
        (everyone, ffn_gain.reshape(-1, LANES), w_up, w_down),
        [VMEM] * 4,
        12,
    )
    terms = lax.all_to_all(term, axes, 0, 0, tiled=True)
    return call(final_kernel, shape((rows, width), BF), (terms, hidden), [VMEM] * 2, 2)


def solution(mesh):
    in_specs = (
        P("dp", ("kv", "tp")),
        P("kv"),
        P("kv", "tp"),
        P("kv", "tp"),
        P("kv", "tp"),
        P("dp", "kv", "tp", None),
        P("dp", "kv", "tp", None),
        P("tp"),
        P(),
        P("tp", "kv"),
        P(),
        P(None, ("dp", "kv", "tp")),
        P(("dp", "kv", "tp"), None),
    )
    out_specs = P("dp", ("kv", "tp"))
    return jax.shard_map(local, mesh=mesh, in_specs=in_specs, out_specs=out_specs, check_vma=False)
```

```python
import functools
import numpy as np
import jax
import jax.numpy as jnp
from jax import lax
from jax.experimental import pallas as pl
from jax.experimental.pallas import tpu as pltpu
from jax.sharding import PartitionSpec as P

D = 4096
HD = 64
VD = 128
EPS = 1e-06
THETA = 500000.0
OUT_SCALE = 0.8
LANES = 128
FAR = -3e38

F32 = jnp.float32
BF = jnp.bfloat16
VMEM = pl.BlockSpec(memory_space=pltpu.VMEM)
SMEM = pl.BlockSpec(memory_space=pltpu.SMEM)
ANY = pl.BlockSpec(memory_space=pl.ANY)


def rounds(count, first):
    if count == 4 and first:
        return ((1, 3, 0, 2), (3, 2, 1, 0), (2, 0, 3, 1))
    return [[(i + step) % count for i in range(count)] for step in reversed(range(1, count))]


def everyones(value, axis, first):
    count = lax.axis_size(axis)
    if count > 8:
        copies = jnp.broadcast_to(value[None], (count,) + value.shape)
        got = lax.all_to_all(copies, axis, 0, 0, tiled=True)
        return [got[k] for k in range(count)]
    got = [value]
    for pairs in rounds(count, first):
        got.append(lax.ppermute(value, axis, list(enumerate(pairs))))
    return got


def rounded(value):
    return value.astype(BF).astype(F32)


def flat_row(ref, first, count):
    return jnp.concatenate([ref[first + i : first + i + 1, :] for i in range(count)], axis=1)


def project_kernel(tokens, other, gain, w_query, w_key, w_value, out):
    first = lax.axis_index("tp") == 0
    own = tokens[...].astype(F32)
    their = other[...].astype(F32)
    slab = jnp.concatenate([jnp.where(first, own, their), jnp.where(first, their, own)], axis=1)
    gains = flat_row(gain[...].astype(F32), 0, gain.shape[0])
    scaled = (slab * gains).astype(BF)
    q = w_query.shape[1]
    k = q + w_key.shape[1]
    v = k + w_value.shape[1]
    out[:, :q] = jnp.dot(scaled, w_query[...], preferred_element_type=F32)
    out[:, q:k] = jnp.dot(scaled, w_key[...], preferred_element_type=F32)
    out[:, k:v] = jnp.dot(scaled, w_value[...], preferred_element_type=F32)
    square = jnp.sum(slab * slab, axis=1, keepdims=True)
    out[:, v:] = jnp.broadcast_to(square, (slab.shape[0], LANES))


def attend_kernel(heads, parts, table, keys, values, out, turn):
    total = parts[0][...]
    for part in parts[1:]:
        total = total + part[...]
    rows = total.shape[0]
    span = 2 * heads
    width = total.shape[1] - LANES
    inverse = lax.rsqrt(total[:, width : width + 1] / D + EPS)
    cosine = table[0:1, :]
    sine = table[1:2, :]
    lane = lax.broadcasted_iota(jnp.int32, (rows, LANES), 1)
    near = lax.rem(lane, HD) < HD // 2

    def rotate(piece):
        ahead = pltpu.roll(piece, LANES - HD // 2, 1)
        behind = pltpu.roll(piece, HD // 2, 1)
        return rounded(piece * cosine + jnp.where(near, ahead, behind) * sine)

    pieces = [total[:, h * LANES : (h + 1) * LANES] * inverse for h in range(heads + 2)]
    for h in range(heads):
        turn[h * rows : (h + 1) * rows, :] = rotate(pieces[h]) * (HD**-0.5)
    new_key = rotate(pieces[heads])
    new_value = rounded(pieces[heads + 1])
    holds_new = lax.axis_index("kv") == 0
    lane_h = lax.broadcasted_iota(jnp.int32, (heads, LANES), 1)
    lane_s = lax.broadcasted_iota(jnp.int32, (span, LANES), 1)
    wide = []
    for r in range(rows):
        mine = turn[pl.ds(r, heads, stride=rows), :]
        wide.append(
            jnp.concatenate(
                [jnp.where(lane_h < HD, mine, 0.0), jnp.where(lane_h < HD, 0.0, mine)], axis=0
            )
        )
    scores = [
        lax.dot_general(
            wide[r].astype(BF), keys[r], (((1,), (1,)), ((), ())), preferred_element_type=F32
        )
        for r in range(rows)
    ]
    own = [
        jnp.where(holds_new, jnp.sum(wide[r] * new_key[r : r + 1, :], axis=1, keepdims=True), FAR)
        for r in range(rows)
    ]
    top = [
        jnp.maximum(jnp.max(scores[r], axis=1, keepdims=True), own[r]) for r in range(rows)
    ]
    weights = [jnp.exp(scores[r] - top[r]) for r in range(rows)]
    own_weight = [jnp.exp(own[r] - top[r]) for r in range(rows)]
    num = [
        jnp.dot(weights[r].astype(BF), values[r], preferred_element_type=F32)
        for r in range(rows)
    ]
    den = [
        jnp.sum(weights[r], axis=1, keepdims=True) + own_weight[r] for r in range(rows)
    ]
    flat = jnp.zeros((span, LANES), F32)
    for r in range(rows):
        flat = jnp.where(lane_s == r, top[r], flat)
        flat = jnp.where(lane_s == rows + r, den[r], flat)
    high = rounded(flat)
    middle = rounded(flat - high)
    low = rounded(flat - high - middle)
    stats = high + pltpu.roll(middle, 2 * rows, 1) + pltpu.roll(low, 4 * rows, 1)
    out[span * rows :, :] = stats.astype(BF)
    for r in range(rows):
        value = num[r] + rounded(own_weight[r]) * new_value[r : r + 1, :]
        out[span * r : span * (r + 1), :] = value.astype(BF)


def merge_kernel(heads, rows, messages, lam, head_gain, w_out, mine, theirs, turn):
    first = lax.axis_index("tp") == 0
    span = 2 * heads
    joined = []
    for message in messages:
        stats = message[span * rows :, :].astype(F32)
        middle = pltpu.roll(stats, LANES - 2 * rows, 1)
        low = pltpu.roll(stats, LANES - 4 * rows, 1)
        joined.append(stats + (middle + low))
    top = functools.reduce(jnp.maximum, joined)
    carried = [jnp.exp(part - top) for part in joined]
    den = sum(c * pltpu.roll(part, LANES - rows, 1) for c, part in zip(carried, joined))
    shares = [c / den for c in carried]
    sub = lax.broadcasted_iota(jnp.int32, (heads, heads), 0)
    across = lax.broadcasted_iota(jnp.int32, (heads, heads), 1)
    lams = jnp.sum(jnp.where(sub == across, lam[...], 0.0), axis=1, keepdims=True)
    gains = head_gain[...].astype(F32) * OUT_SCALE
    mixes = []
    for r in range(rows):
        ratio = sum(
            share[:, r : r + 1] * message[span * r : span * (r + 1), :].astype(F32)
            for share, message in zip(shares, messages)
        )
        mixes.append(ratio[:heads] - lams * ratio[heads:])
    means = [jnp.mean(mix * mix, axis=1, keepdims=True) for mix in mixes]
    for r in range(rows):
        turn[r * heads : (r + 1) * heads, :] = mixes[r] * lax.rsqrt(means[r] + EPS) * gains
    wide = jnp.concatenate(
        [turn[pl.ds(h, rows, stride=heads), :] for h in range(heads)], axis=1
    )
    branch = jnp.dot(wide.astype(BF), w_out[...], preferred_element_type=F32)
    half = branch.shape[1] // 2
    mine[...] = jnp.where(first, branch[:, :half], branch[:, half:]).astype(BF)
    theirs[...] = jnp.where(first, branch[:, half:], branch[:, :half]).astype(BF)


def hidden_kernel(tokens, mine, received, copies, hidden):
    branch = mine[...].astype(F32) + received[...].astype(F32)
    value = (tokens[...].astype(F32) + branch).astype(BF)
    hidden[...] = value
    for k in range(copies.shape[0]):
        copies[k] = value


def mixer_kernel(dps, everyone, gain, w_up, w_down, out):
    devices, rows, width = everyone.shape
    blocks = devices // dps
    per = width // LANES
    gains = gain[...].astype(F32)
    square = jnp.zeros((dps * rows, width), F32)
    upward = jnp.zeros((dps * rows, w_up.shape[1]), F32)
    for b in range(blocks):
        block = jnp.concatenate(
            [everyone[a * blocks + b].astype(F32) for a in range(dps)], axis=0
        )
        square = square + block * block
        scaled = (block * flat_row(gains, b * per, per)).astype(BF)
        upward = upward + jnp.dot(
            scaled, w_up[b * width : (b + 1) * width, :], preferred_element_type=F32
        )
    inverse = lax.rsqrt(jnp.sum(square, axis=1, keepdims=True) / D + EPS)
    act = jnp.square(jnp.maximum(upward * inverse, 0.0)).astype(BF)
    for b in range(blocks):
        down = jnp.dot(
            act, w_down[:, b * width : (b + 1) * width], preferred_element_type=F32
        ).astype(BF)
        for a in range(dps):
            out[a * blocks + b] = down[a * rows : (a + 1) * rows, :]


def final_kernel(terms, hidden, out):
    total = terms[0].astype(F32)
    for k in range(1, terms.shape[0]):
        total = total + terms[k].astype(F32)
    out[...] = (hidden[...].astype(F32) + total).astype(BF)


def load_kernel(count, *refs):
    sources, held, sems = refs[:count], refs[count : 2 * count], refs[2 * count]
    copies = [
        pltpu.make_async_copy(source, target, sems.at[i])
        for i, (source, target) in enumerate(zip(sources, held))
    ]
    for copy in copies:
        copy.start()
    for copy in copies:
        copy.wait()


def loaded(*arrays):
    count = len(arrays)
    return pl.pallas_call(
        functools.partial(load_kernel, count),
        out_shape=[jax.ShapeDtypeStruct(array.shape, array.dtype) for array in arrays],
        in_specs=[pl.BlockSpec(memory_space=pltpu.HBM)] * count,
        out_specs=[VMEM] * count,
        scratch_shapes=[pltpu.SemaphoreType.DMA((count,))],
        compiler_params=pltpu.CompilerParams(vmem_limit_bytes=1 << 20),
        cost_estimate=pl.CostEstimate(
            flops=8 << 30, bytes_accessed=8 << 20, transcendentals=0
        ),
    )(*(pltpu.with_memory_space_constraint(array, pltpu.HBM) for array in arrays))


def tables(position):
    half = HD // 2
    angle = position * THETA ** (-np.arange(half, dtype=np.float64) * 2.0 / HD)
    cosine = np.tile(np.cos(angle), LANES // half)
    sine = np.tile(np.concatenate([-np.sin(angle), np.sin(angle)]), LANES // HD)
    rest = np.zeros((6, LANES))
    return jnp.asarray(np.concatenate([cosine[None], sine[None], rest]), F32)


def call(kernel, shapes, inputs, mib, cost=1, scratch=()):
    return pl.pallas_call(
        kernel,
        out_shape=shapes,
        in_specs=[VMEM] * len(inputs),
        out_specs=jax.tree.map(lambda _: VMEM, shapes),
        scratch_shapes=[pltpu.VMEM(shape, F32) for shape in scratch],
        compiler_params=pltpu.CompilerParams(vmem_limit_bytes=mib << 20),
        cost_estimate=pl.CostEstimate(
            flops=cost << 30, bytes_accessed=cost << 20, transcendentals=0
        ),
    )(*inputs)


def local(
    tokens,
    attn_gain,
    w_query,
    w_key,
    w_value,
    key_cache,
    value_cache,
    lam,
    head_gain,
    w_out,
    ffn_gain,
    w_up,
    w_down,
):
    rows, width = tokens.shape
    kv_count = lax.axis_size("kv")
    tp_count = lax.axis_size("tp")
    dp_count = lax.axis_size("dp")
    positions = key_cache.shape[1]
    heads = lam.shape[0]
    axes = ("dp", "kv", "tp")
    swap = [(0, 1), (1, 0)]
    assert tp_count == 2 and key_cache.shape[2] == 1 and 6 * rows <= LANES
    shape = jax.ShapeDtypeStruct

    other = lax.ppermute(tokens, "tp", swap)
    packed = w_query.shape[1] + w_key.shape[1] + w_value.shape[1] + LANES
    held, gain = loaded(tokens, attn_gain.reshape(-1, LANES))
    part = call(
        project_kernel,
        shape((rows, packed), F32),
        (held, other, gain, w_query, w_key, w_value),
        6,
        8,
    )
    parts = everyones(part, "kv", True)
    count = len(parts)

    def attend(*refs):
        attend_kernel(heads, refs[:count], *refs[count:])

    message = call(
        attend,
        shape((2 * heads * (rows + 1), LANES), BF),
        (
            *parts,
            tables(positions * kv_count),
            key_cache.reshape(rows, positions, 2 * HD),
            value_cache.reshape(rows, positions, VD),
        ),
        8,
        8,
        [(heads * rows, LANES)],
    )
    messages = everyones(message, "kv", False)

    def merge(*refs):
        merge_kernel(heads, rows, refs[:count], *refs[count:])

    mine, theirs = call(
        merge,
        (shape((rows, width), BF), shape((rows, width), BF)),
        (*messages, lam.reshape(1, heads), head_gain.reshape(1, VD), w_out),
        5,
        8,
        [(heads * rows, LANES)],
    )
    received = lax.ppermute(theirs, "tp", swap)
    devices = dp_count * kv_count * tp_count
    copies, hidden = call(
        hidden_kernel,
        (shape((devices, rows, width), BF), shape((rows, width), BF)),
        (held, mine, received),
        2,
    )
    everyone = lax.all_to_all(copies, axes, 0, 0, tiled=True)
    term = call(
        functools.partial(mixer_kernel, dp_count),
        shape((devices, rows, width), BF),
        (everyone, ffn_gain.reshape(-1, LANES), w_up, w_down),
        12,
    )
    terms = lax.all_to_all(term, axes, 0, 0, tiled=True)
    return call(final_kernel, shape((rows, width), BF), (terms, hidden), 2)


def solution(mesh):
    in_specs = (
        P("dp", ("kv", "tp")),
        P("kv"),
        P("kv", "tp"),
        P("kv", "tp"),
        P("kv", "tp"),
        P("dp", "kv", "tp", None),
        P("dp", "kv", "tp", None),
        P("tp"),
        P(),
        P("tp", "kv"),
        P(),
        P(None, ("dp", "kv", "tp")),
        P(("dp", "kv", "tp"), None),
    )
    out_specs = P("dp", ("kv", "tp"))
    return jax.shard_map(local, mesh=mesh, in_specs=in_specs, out_specs=out_specs, check_vma=False)
```

```python
import functools
import numpy as np
import jax
import jax.numpy as jnp
from jax import lax
from jax.experimental import pallas as pl
from jax.experimental.pallas import tpu as pltpu
from jax.sharding import PartitionSpec as P

D = 4096
HD = 64
VD = 128
EPS = 1e-06
THETA = 500000.0
OUT_SCALE = 0.8
LANES = 128
FAR = -3e38

F32 = jnp.float32
BF = jnp.bfloat16
VMEM = pl.BlockSpec(memory_space=pltpu.VMEM)
SMEM = pl.BlockSpec(memory_space=pltpu.SMEM)
ANY = pl.BlockSpec(memory_space=pl.ANY)


def rounds(count, first):
    if count == 4 and first:
        return ((1, 3, 0, 2), (3, 2, 1, 0), (2, 0, 3, 1))
    return [[(i + step) % count for i in range(count)] for step in reversed(range(1, count))]


def everyones(value, axis, first):
    count = lax.axis_size(axis)
    if count > 8:
        copies = jnp.broadcast_to(value[None], (count,) + value.shape)
        got = lax.all_to_all(copies, axis, 0, 0, tiled=True)
        return [got[k] for k in range(count)]
    got = [value]
    for pairs in rounds(count, first):
        got.append(lax.ppermute(value, axis, list(enumerate(pairs))))
    return got


def rounded(value):
    return value.astype(BF).astype(F32)


def flat_row(ref, first, count):
    return jnp.concatenate([ref[first + i : first + i + 1, :] for i in range(count)], axis=1)


def project_kernel(tokens, other, gain, w_query, w_key, w_value, out):
    first = lax.axis_index("tp") == 0
    own = tokens[...].astype(F32)
    their = other[...].astype(F32)
    slab = jnp.concatenate([jnp.where(first, own, their), jnp.where(first, their, own)], axis=1)
    gains = flat_row(gain[...].astype(F32), 0, gain.shape[0])
    scaled = (slab * gains).astype(BF)
    q = w_query.shape[1]
    k = q + w_key.shape[1]
    v = k + w_value.shape[1]
    out[:, :q] = jnp.dot(scaled, w_query[...], preferred_element_type=F32)
    out[:, q:k] = jnp.dot(scaled, w_key[...], preferred_element_type=F32)
    out[:, k:v] = jnp.dot(scaled, w_value[...], preferred_element_type=F32)
    square = jnp.sum(slab * slab, axis=1, keepdims=True)
    out[:, v:] = jnp.broadcast_to(square, (slab.shape[0], LANES))


def attend_kernel(heads, parts, table, keys, values, out, turn):
    total = parts[0][...]
    for part in parts[1:]:
        total = total + part[...]
    rows = total.shape[0]
    span = 2 * heads
    width = total.shape[1] - LANES
    inverse = lax.rsqrt(total[:, width : width + 1] / D + EPS)
    cosine = table[0:1, :]
    sine = table[1:2, :]
    lane = lax.broadcasted_iota(jnp.int32, (rows, LANES), 1)
    near = lax.rem(lane, HD) < HD // 2

    def rotate(piece):
        ahead = pltpu.roll(piece, LANES - HD // 2, 1)
        behind = pltpu.roll(piece, HD // 2, 1)
        return rounded(piece * cosine + jnp.where(near, ahead, behind) * sine)

    pieces = [total[:, h * LANES : (h + 1) * LANES] * inverse for h in range(heads + 2)]
    for h in range(heads):
        turn[h * rows : (h + 1) * rows, :] = rotate(pieces[h]) * (HD**-0.5)
    new_key = rotate(pieces[heads])
    new_value = rounded(pieces[heads + 1])
    holds_new = lax.axis_index("kv") == 0
    lane_h = lax.broadcasted_iota(jnp.int32, (heads, LANES), 1)
    lane_s = lax.broadcasted_iota(jnp.int32, (span, LANES), 1)
    wide = []
    for r in range(rows):
        mine = turn[pl.ds(r, heads, stride=rows), :]
        wide.append(
            jnp.concatenate(
                [jnp.where(lane_h < HD, mine, 0.0), jnp.where(lane_h < HD, 0.0, mine)], axis=0
            )
        )
    scores = [
        lax.dot_general(
            wide[r].astype(BF), keys[r], (((1,), (1,)), ((), ())), preferred_element_type=F32
        )
        for r in range(rows)
    ]
    own = [
        jnp.where(holds_new, jnp.sum(wide[r] * new_key[r : r + 1, :], axis=1, keepdims=True), FAR)
        for r in range(rows)
    ]
    top = [
        jnp.maximum(jnp.max(scores[r], axis=1, keepdims=True), own[r]) for r in range(rows)
    ]
    weights = [jnp.exp(scores[r] - top[r]) for r in range(rows)]
    own_weight = [jnp.exp(own[r] - top[r]) for r in range(rows)]
    num = [
        jnp.dot(weights[r].astype(BF), values[r], preferred_element_type=F32)
        for r in range(rows)
    ]
    den = [
        jnp.sum(weights[r], axis=1, keepdims=True) + own_weight[r] for r in range(rows)
    ]
    flat = jnp.zeros((span, LANES), F32)
    for r in range(rows):
        flat = jnp.where(lane_s == r, top[r], flat)
        flat = jnp.where(lane_s == rows + r, den[r], flat)
    high = rounded(flat)
    middle = rounded(flat - high)
    low = rounded(flat - high - middle)
    stats = high + pltpu.roll(middle, 2 * rows, 1) + pltpu.roll(low, 4 * rows, 1)
    out[span * rows :, :] = stats.astype(BF)
    for r in range(rows):
        value = num[r] + rounded(own_weight[r]) * new_value[r : r + 1, :]
        out[span * r : span * (r + 1), :] = value.astype(BF)


def merge_kernel(heads, rows, messages, lam, head_gain, w_out, attended, theirs, turn):
    span = 2 * heads
    joined = []
    for message in messages:
        stats = message[span * rows :, :].astype(F32)
        middle = pltpu.roll(stats, LANES - 2 * rows, 1)
        low = pltpu.roll(stats, LANES - 4 * rows, 1)
        joined.append(stats + (middle + low))
    top = functools.reduce(jnp.maximum, joined)
    carried = [jnp.exp(part - top) for part in joined]
    den = sum(c * pltpu.roll(part, LANES - rows, 1) for c, part in zip(carried, joined))
    shares = [c / den for c in carried]
    sub = lax.broadcasted_iota(jnp.int32, (heads, heads), 0)
    across = lax.broadcasted_iota(jnp.int32, (heads, heads), 1)
    lams = jnp.sum(jnp.where(sub == across, lam[...], 0.0), axis=1, keepdims=True)
    gains = head_gain[...].astype(F32) * OUT_SCALE
    mixes = []
    for r in range(rows):
        ratio = sum(
            share[:, r : r + 1] * message[span * r : span * (r + 1), :].astype(F32)
            for share, message in zip(shares, messages)
        )
        mixes.append(ratio[:heads] - lams * ratio[heads:])
    means = [jnp.mean(mix * mix, axis=1, keepdims=True) for mix in mixes]
    for r in range(rows):
        turn[r * heads : (r + 1) * heads, :] = mixes[r] * lax.rsqrt(means[r] + EPS) * gains
    wide = jnp.concatenate(
        [turn[pl.ds(h, rows, stride=heads), :] for h in range(heads)], axis=1
    )
    half = theirs.shape[1]
    at = pl.ds(pl.multiple_of((1 - lax.axis_index("tp")) * half, LANES), half)
    wide = wide.astype(BF)
    theirs[...] = jnp.dot(wide, w_out[:, at], preferred_element_type=F32).astype(BF)
    attended[...] = wide


def branch_kernel(tokens, attended, w_out, out):
    half = out.shape[1] // 2
    at = pl.ds(pl.multiple_of(lax.axis_index("tp") * half, LANES), half)
    branch = jnp.dot(attended[...], w_out[:, at], preferred_element_type=F32).astype(BF)
    out[:, :half] = branch.astype(F32)
    out[:, half:] = tokens[...].astype(F32)


def hidden_kernel(base, received, copies, hidden):
    half = hidden.shape[1]
    branch = base[:, :half] + received[...].astype(F32)
    value = (base[:, half:] + branch).astype(BF)
    hidden[...] = value
    for k in range(copies.shape[0]):
        copies[k] = value


def mixer_kernel(dps, everyone, gain, w_up, w_down, out):
    devices, rows, width = everyone.shape
    blocks = devices // dps
    per = width // LANES
    gains = gain[...].astype(F32)
    square = jnp.zeros((dps * rows, width), F32)
    upward = jnp.zeros((dps * rows, w_up.shape[1]), F32)
    for b in range(blocks):
        block = jnp.concatenate(
            [everyone[a * blocks + b].astype(F32) for a in range(dps)], axis=0
        )
        square = square + block * block
        scaled = (block * flat_row(gains, b * per, per)).astype(BF)
        upward = upward + jnp.dot(
            scaled, w_up[b * width : (b + 1) * width, :], preferred_element_type=F32
        )
    inverse = lax.rsqrt(jnp.sum(square, axis=1, keepdims=True) / D + EPS)
    act = jnp.square(jnp.maximum(upward * inverse, 0.0)).astype(BF)
    for b in range(blocks):
        down = jnp.dot(
            act, w_down[:, b * width : (b + 1) * width], preferred_element_type=F32
        ).astype(BF)
        for a in range(dps):
            out[a * blocks + b] = down[a * rows : (a + 1) * rows, :]


def final_kernel(terms, hidden, out):
    total = terms[0].astype(F32)
    for k in range(1, terms.shape[0]):
        total = total + terms[k].astype(F32)
    out[...] = (hidden[...].astype(F32) + total).astype(BF)


def load_kernel(count, *refs):
    sources, held, sems = refs[:count], refs[count : 2 * count], refs[2 * count]
    copies = [
        pltpu.make_async_copy(source, target, sems.at[i])
        for i, (source, target) in enumerate(zip(sources, held))
    ]
    for copy in copies:
        copy.start()
    for copy in copies:
        copy.wait()


def loaded(*arrays):
    count = len(arrays)
    return pl.pallas_call(
        functools.partial(load_kernel, count),
        out_shape=[jax.ShapeDtypeStruct(array.shape, array.dtype) for array in arrays],
        in_specs=[pl.BlockSpec(memory_space=pltpu.HBM)] * count,
        out_specs=[VMEM] * count,
        scratch_shapes=[pltpu.SemaphoreType.DMA((count,))],
        compiler_params=pltpu.CompilerParams(vmem_limit_bytes=1 << 20),
        cost_estimate=pl.CostEstimate(
            flops=8 << 30, bytes_accessed=8 << 20, transcendentals=0
        ),
    )(*(pltpu.with_memory_space_constraint(array, pltpu.HBM) for array in arrays))


def tables(position):
    half = HD // 2
    angle = position * THETA ** (-np.arange(half, dtype=np.float64) * 2.0 / HD)
    cosine = np.tile(np.cos(angle), LANES // half)
    sine = np.tile(np.concatenate([-np.sin(angle), np.sin(angle)]), LANES // HD)
    rest = np.zeros((6, LANES))
    return jnp.asarray(np.concatenate([cosine[None], sine[None], rest]), F32)


def call(kernel, shapes, inputs, mib, cost=1, scratch=()):
    return pl.pallas_call(
        kernel,
        out_shape=shapes,
        in_specs=[VMEM] * len(inputs),
        out_specs=jax.tree.map(lambda _: VMEM, shapes),
        scratch_shapes=[pltpu.VMEM(shape, F32) for shape in scratch],
        compiler_params=pltpu.CompilerParams(vmem_limit_bytes=mib << 20),
        cost_estimate=pl.CostEstimate(
            flops=cost << 30, bytes_accessed=cost << 20, transcendentals=0
        ),
    )(*inputs)


def local(
    tokens,
    attn_gain,
    w_query,
    w_key,
    w_value,
    key_cache,
    value_cache,
    lam,
    head_gain,
    w_out,
    ffn_gain,
    w_up,
    w_down,
):
    rows, width = tokens.shape
    kv_count = lax.axis_size("kv")
    tp_count = lax.axis_size("tp")
    dp_count = lax.axis_size("dp")
    positions = key_cache.shape[1]
    heads = lam.shape[0]
    axes = ("dp", "kv", "tp")
    swap = [(0, 1), (1, 0)]
    assert tp_count == 2 and key_cache.shape[2] == 1 and 6 * rows <= LANES
    shape = jax.ShapeDtypeStruct

    other = lax.ppermute(tokens, "tp", swap)
    packed = w_query.shape[1] + w_key.shape[1] + w_value.shape[1] + LANES
    held, gain = loaded(tokens, attn_gain.reshape(-1, LANES))
    part = call(
        project_kernel,
        shape((rows, packed), F32),
        (held, other, gain, w_query, w_key, w_value),
        6,
        8,
    )
    parts = everyones(part, "kv", True)
    count = len(parts)

    def attend(*refs):
        attend_kernel(heads, refs[:count], *refs[count:])

    message = call(
        attend,
        shape((2 * heads * (rows + 1), LANES), BF),
        (
            *parts,
            tables(positions * kv_count),
            key_cache.reshape(rows, positions, 2 * HD),
            value_cache.reshape(rows, positions, VD),
        ),
        8,
        8,
        [(heads * rows, LANES)],
    )
    messages = everyones(message, "kv", False)

    def merge(*refs):
        merge_kernel(heads, rows, refs[:count], *refs[count:])

    attended, theirs = call(
        merge,
        (shape((rows, heads * VD), BF), shape((rows, width), BF)),
        (*messages, lam.reshape(1, heads), head_gain.reshape(1, VD), w_out),
        5,
        8,
        [(heads * rows, LANES)],
    )
    received = lax.ppermute(theirs, "tp", swap)
    base = call(branch_kernel, shape((rows, 2 * width), F32), (held, attended, w_out), 5)
    devices = dp_count * kv_count * tp_count
    copies, hidden = call(
        hidden_kernel,
        (shape((devices, rows, width), BF), shape((rows, width), BF)),
        (base, received),
        2,
    )
    everyone = lax.all_to_all(copies, axes, 0, 0, tiled=True)
    term = call(
        functools.partial(mixer_kernel, dp_count),
        shape((devices, rows, width), BF),
        (everyone, ffn_gain.reshape(-1, LANES), w_up, w_down),
        12,
    )
    terms = lax.all_to_all(term, axes, 0, 0, tiled=True)
    return call(final_kernel, shape((rows, width), BF), (terms, hidden), 2)


def solution(mesh):
    in_specs = (
        P("dp", ("kv", "tp")),
        P("kv"),
        P("kv", "tp"),
        P("kv", "tp"),
        P("kv", "tp"),
        P("dp", "kv", "tp", None),
        P("dp", "kv", "tp", None),
        P("tp"),
        P(),
        P("tp", "kv"),
        P(),
        P(None, ("dp", "kv", "tp")),
        P(("dp", "kv", "tp"), None),
    )
    out_specs = P("dp", ("kv", "tp"))
    return jax.shard_map(local, mesh=mesh, in_specs=in_specs, out_specs=out_specs, check_vma=False)
```

```python
import functools
import numpy as np
import jax
import jax.numpy as jnp
from jax import lax
from jax.experimental import pallas as pl
from jax.experimental.pallas import tpu as pltpu
from jax.sharding import PartitionSpec as P

D = 4096
HD = 64
VD = 128
EPS = 1e-06
THETA = 500000.0
OUT_SCALE = 0.8
LANES = 128
FAR = -3e38

F32 = jnp.float32
BF = jnp.bfloat16
VMEM = pl.BlockSpec(memory_space=pltpu.VMEM)


def rounds(count, first):
    if count == 4 and first:
        return ((1, 3, 0, 2), (3, 2, 1, 0), (2, 0, 3, 1))
    return [[(i + step) % count for i in range(count)] for step in reversed(range(1, count))]


def everyones(value, axis, first):
    count = lax.axis_size(axis)
    if count > 8:
        copies = jnp.broadcast_to(value[None], (count,) + value.shape)
        got = lax.all_to_all(copies, axis, 0, 0, tiled=True)
        return [got[k] for k in range(count)]
    got = [value]
    for pairs in rounds(count, first):
        got.append(lax.ppermute(value, axis, list(enumerate(pairs))))
    return got


def rounded(value):
    return value.astype(BF).astype(F32)


def flat_row(ref, first, count):
    return jnp.concatenate([ref[first + i : first + i + 1, :] for i in range(count)], axis=1)


def project_kernel(tokens, other, gain, w_query, w_key, w_value, out):
    first = lax.axis_index("tp") == 0
    own = tokens[...].astype(F32)
    their = other[...].astype(F32)
    slab = jnp.concatenate([jnp.where(first, own, their), jnp.where(first, their, own)], axis=1)
    gains = flat_row(gain[...].astype(F32), 0, gain.shape[0])
    scaled = (slab * gains).astype(BF)
    q = w_query.shape[1]
    k = q + w_key.shape[1]
    v = k + w_value.shape[1]
    out[:, :q] = jnp.dot(scaled, w_query[...], preferred_element_type=F32)
    out[:, q:k] = jnp.dot(scaled, w_key[...], preferred_element_type=F32)
    out[:, k:v] = jnp.dot(scaled, w_value[...], preferred_element_type=F32)
    square = jnp.sum(slab * slab, axis=1, keepdims=True)
    out[:, v:] = jnp.broadcast_to(square, (slab.shape[0], LANES))


def attend_kernel(heads, parts, table, keys, values, out, turn):
    total = parts[0][...]
    for part in parts[1:]:
        total = total + part[...]
    rows = total.shape[0]
    span = 2 * heads
    width = total.shape[1] - LANES
    inverse = lax.rsqrt(total[:, width : width + 1] / D + EPS)
    cosine = table[0:1, :]
    sine = table[1:2, :]
    lane = lax.broadcasted_iota(jnp.int32, (rows, LANES), 1)
    near = lax.rem(lane, HD) < HD // 2

    def rotate(piece):
        ahead = pltpu.roll(piece, LANES - HD // 2, 1)
        behind = pltpu.roll(piece, HD // 2, 1)
        return rounded(piece * cosine + jnp.where(near, ahead, behind) * sine)

    pieces = [total[:, h * LANES : (h + 1) * LANES] * inverse for h in range(heads + 2)]
    for h in range(heads):
        turn[h * rows : (h + 1) * rows, :] = rotate(pieces[h]) * (HD**-0.5)
    new_key = rotate(pieces[heads])
    new_value = rounded(pieces[heads + 1])
    holds_new = lax.axis_index("kv") == 0
    lane_h = lax.broadcasted_iota(jnp.int32, (heads, LANES), 1)
    lane_s = lax.broadcasted_iota(jnp.int32, (span, LANES), 1)
    wide = []
    for r in range(rows):
        mine = turn[pl.ds(r, heads, stride=rows), :]
        wide.append(
            jnp.concatenate(
                [jnp.where(lane_h < HD, mine, 0.0), jnp.where(lane_h < HD, 0.0, mine)], axis=0
            )
        )
    scores = [
        lax.dot_general(
            wide[r].astype(BF), keys[r], (((1,), (1,)), ((), ())), preferred_element_type=F32
        )
        for r in range(rows)
    ]
    own = [
        jnp.where(holds_new, jnp.sum(wide[r] * new_key[r : r + 1, :], axis=1, keepdims=True), FAR)
        for r in range(rows)
    ]
    top = [
        jnp.maximum(jnp.max(scores[r], axis=1, keepdims=True), own[r]) for r in range(rows)
    ]
    weights = [jnp.exp(scores[r] - top[r]) for r in range(rows)]
    own_weight = [jnp.exp(own[r] - top[r]) for r in range(rows)]
    num = [
        jnp.dot(weights[r].astype(BF), values[r], preferred_element_type=F32)
        for r in range(rows)
    ]
    den = [
        jnp.sum(weights[r], axis=1, keepdims=True) + own_weight[r] for r in range(rows)
    ]
    flat = jnp.zeros((span, LANES), F32)
    for r in range(rows):
        flat = jnp.where(lane_s == r, top[r], flat)
        flat = jnp.where(lane_s == rows + r, den[r], flat)
    high = rounded(flat)
    middle = rounded(flat - high)
    low = rounded(flat - high - middle)
    stats = high + pltpu.roll(middle, 2 * rows, 1) + pltpu.roll(low, 4 * rows, 1)
    out[span * rows :, :] = stats.astype(BF)
    for r in range(rows):
        value = num[r] + rounded(own_weight[r]) * new_value[r : r + 1, :]
        out[span * r : span * (r + 1), :] = value.astype(BF)


def merge_kernel(heads, rows, messages, lam, head_gain, w_out, attended, theirs, turn):
    span = 2 * heads
    joined = []
    for message in messages:
        stats = message[span * rows :, :].astype(F32)
        middle = pltpu.roll(stats, LANES - 2 * rows, 1)
        low = pltpu.roll(stats, LANES - 4 * rows, 1)
        joined.append(stats + (middle + low))
    top = functools.reduce(jnp.maximum, joined)
    carried = [jnp.exp(part - top) for part in joined]
    den = sum(c * pltpu.roll(part, LANES - rows, 1) for c, part in zip(carried, joined))
    shares = [c / den for c in carried]
    sub = lax.broadcasted_iota(jnp.int32, (heads, heads), 0)
    across = lax.broadcasted_iota(jnp.int32, (heads, heads), 1)
    lams = jnp.sum(jnp.where(sub == across, lam[...], 0.0), axis=1, keepdims=True)
    gains = head_gain[...].astype(F32) * OUT_SCALE
    mixes = []
    for r in range(rows):
        ratio = sum(
            share[:, r : r + 1] * message[span * r : span * (r + 1), :].astype(F32)
            for share, message in zip(shares, messages)
        )
        mixes.append(ratio[:heads] - lams * ratio[heads:])
    means = [jnp.mean(mix * mix, axis=1, keepdims=True) for mix in mixes]
    for r in range(rows):
        turn[r * heads : (r + 1) * heads, :] = mixes[r] * lax.rsqrt(means[r] + EPS) * gains
    wide = jnp.concatenate(
        [turn[pl.ds(h, rows, stride=heads), :] for h in range(heads)], axis=1
    )
    half = theirs.shape[1]
    at = pl.ds(pl.multiple_of((1 - lax.axis_index("tp")) * half, LANES), half)
    wide = wide.astype(BF)
    theirs[...] = jnp.dot(wide, w_out[:, at], preferred_element_type=F32).astype(BF)
    attended[...] = wide


def branch_kernel(tokens, attended, w_out, out):
    half = out.shape[1] // 2
    at = pl.ds(pl.multiple_of(lax.axis_index("tp") * half, LANES), half)
    branch = jnp.dot(attended[...], w_out[:, at], preferred_element_type=F32).astype(BF)
    out[:, :half] = branch.astype(F32)
    out[:, half:] = tokens[...].astype(F32)


def hidden_kernel(base, received, copies, hidden):
    half = hidden.shape[1]
    branch = base[:, :half] + received[...].astype(F32)
    value = (base[:, half:] + branch).astype(BF)
    hidden[...] = value
    for k in range(copies.shape[0]):
        copies[k] = value


def mixer_kernel(dps, everyone, gain, w_up, w_down, out):
    devices, rows, width = everyone.shape
    blocks = devices // dps
    per = width // LANES
    places = [(b % 2 * (blocks // 2) + b // 2) * dps for b in range(blocks)]
    gains = gain[...].astype(F32)
    square = jnp.zeros((dps * rows, width), F32)
    upward = jnp.zeros((dps * rows, w_up.shape[1]), F32)
    for b in range(blocks):
        block = jnp.concatenate(
            [everyone[places[b] + a].astype(F32) for a in range(dps)], axis=0
        )
        square = square + block * block
        scaled = (block * flat_row(gains, b * per, per)).astype(BF)
        upward = upward + jnp.dot(
            scaled, w_up[b * width : (b + 1) * width, :], preferred_element_type=F32
        )
    inverse = lax.rsqrt(jnp.sum(square, axis=1, keepdims=True) / D + EPS)
    act = jnp.square(jnp.maximum(upward * inverse, 0.0)).astype(BF)
    for b in range(blocks):
        down = jnp.dot(
            act, w_down[:, b * width : (b + 1) * width], preferred_element_type=F32
        ).astype(BF)
        for a in range(dps):
            out[places[b] + a] = down[a * rows : (a + 1) * rows, :]


def final_kernel(terms, hidden, out):
    total = terms[0].astype(F32)
    for k in range(1, terms.shape[0]):
        total = total + terms[k].astype(F32)
    out[...] = (hidden[...].astype(F32) + total).astype(BF)


def load_kernel(count, *refs):
    sources, held, sems = refs[:count], refs[count : 2 * count], refs[2 * count]
    copies = [
        pltpu.make_async_copy(source, target, sems.at[i])
        for i, (source, target) in enumerate(zip(sources, held))
    ]
    for copy in copies:
        copy.start()
    for copy in copies:
        copy.wait()


def loaded(*arrays):
    count = len(arrays)
    return pl.pallas_call(
        functools.partial(load_kernel, count),
        out_shape=[jax.ShapeDtypeStruct(array.shape, array.dtype) for array in arrays],
        in_specs=[pl.BlockSpec(memory_space=pltpu.HBM)] * count,
        out_specs=[VMEM] * count,
        scratch_shapes=[pltpu.SemaphoreType.DMA((count,))],
        compiler_params=pltpu.CompilerParams(vmem_limit_bytes=1 << 20),
        cost_estimate=pl.CostEstimate(
            flops=8 << 30, bytes_accessed=8 << 20, transcendentals=0
        ),
    )(*(pltpu.with_memory_space_constraint(array, pltpu.HBM) for array in arrays))


def tables(position):
    half = HD // 2
    angle = position * THETA ** (-np.arange(half, dtype=np.float64) * 2.0 / HD)
    cosine = np.tile(np.cos(angle), LANES // half)
    sine = np.tile(np.concatenate([-np.sin(angle), np.sin(angle)]), LANES // HD)
    rest = np.zeros((6, LANES))
    return jnp.asarray(np.concatenate([cosine[None], sine[None], rest]), F32)


def call(kernel, shapes, inputs, mib, cost=1, scratch=()):
    return pl.pallas_call(
        kernel,
        out_shape=shapes,
        in_specs=[VMEM] * len(inputs),
        out_specs=jax.tree.map(lambda _: VMEM, shapes),
        scratch_shapes=[pltpu.VMEM(shape, F32) for shape in scratch],
        compiler_params=pltpu.CompilerParams(vmem_limit_bytes=mib << 20),
        cost_estimate=pl.CostEstimate(
            flops=cost << 30, bytes_accessed=cost << 20, transcendentals=0
        ),
    )(*inputs)


def local(
    tokens,
    attn_gain,
    w_query,
    w_key,
    w_value,
    key_cache,
    value_cache,
    lam,
    head_gain,
    w_out,
    ffn_gain,
    w_up,
    w_down,
):
    rows, width = tokens.shape
    kv_count = lax.axis_size("kv")
    tp_count = lax.axis_size("tp")
    dp_count = lax.axis_size("dp")
    positions = key_cache.shape[1]
    heads = lam.shape[0]
    axes = ("tp", "kv", "dp")
    swap = [(0, 1), (1, 0)]
    assert tp_count == 2 and key_cache.shape[2] == 1 and 6 * rows <= LANES
    shape = jax.ShapeDtypeStruct

    other = lax.ppermute(tokens, "tp", swap)
    packed = w_query.shape[1] + w_key.shape[1] + w_value.shape[1] + LANES
    held, gain = loaded(tokens, attn_gain.reshape(-1, LANES))
    part = call(
        project_kernel,
        shape((rows, packed), F32),
        (held, other, gain, w_query, w_key, w_value),
        6,
        8,
    )
    parts = everyones(part, "kv", True)
    count = len(parts)

    def attend(*refs):
        attend_kernel(heads, refs[:count], *refs[count:])

    message = call(
        attend,
        shape((2 * heads * (rows + 1), LANES), BF),
        (
            *parts,
            tables(positions * kv_count),
            key_cache.reshape(rows, positions, 2 * HD),
            value_cache.reshape(rows, positions, VD),
        ),
        8,
        8,
        [(heads * rows, LANES)],
    )
    messages = everyones(message, "kv", False)

    def merge(*refs):
        merge_kernel(heads, rows, refs[:count], *refs[count:])

    attended, theirs = call(
        merge,
        (shape((rows, heads * VD), BF), shape((rows, width), BF)),
        (*messages, lam.reshape(1, heads), head_gain.reshape(1, VD), w_out),
        5,
        8,
        [(heads * rows, LANES)],
    )
    received = lax.ppermute(theirs, "tp", swap)
    base = call(branch_kernel, shape((rows, 2 * width), F32), (held, attended, w_out), 5)
    devices = dp_count * kv_count * tp_count
    copies, hidden = call(
        hidden_kernel,
        (shape((devices, rows, width), BF), shape((rows, width), BF)),
        (base, received),
        2,
    )
    everyone = lax.all_to_all(copies, axes, 0, 0, tiled=True)
    term = call(
        functools.partial(mixer_kernel, dp_count),
        shape((devices, rows, width), BF),
        (everyone, ffn_gain.reshape(-1, LANES), w_up, w_down),
        12,
    )
    terms = lax.all_to_all(term, axes, 0, 0, tiled=True)
    return call(final_kernel, shape((rows, width), BF), (terms, hidden), 2)


def solution(mesh):
    in_specs = (
        P("dp", ("kv", "tp")),
        P("kv"),
        P("kv", "tp"),
        P("kv", "tp"),
        P("kv", "tp"),
        P("dp", "kv", "tp", None),
        P("dp", "kv", "tp", None),
        P("tp"),
        P(),
        P("tp", "kv"),
        P(),
        P(None, ("dp", "kv", "tp")),
        P(("dp", "kv", "tp"), None),
    )
    out_specs = P("dp", ("kv", "tp"))
    return jax.shard_map(local, mesh=mesh, in_specs=in_specs, out_specs=out_specs, check_vma=False)
```

```python
import functools
import numpy as np
import jax
import jax.numpy as jnp
from jax import lax
from jax.experimental import pallas as pl
from jax.experimental.pallas import tpu as pltpu
from jax.sharding import PartitionSpec as P

D = 4096
HD = 64
VD = 128
EPS = 1e-06
THETA = 500000.0
OUT_SCALE = 0.8
LANES = 128
FAR = -3e38

F32 = jnp.float32
BF = jnp.bfloat16
VMEM = pl.BlockSpec(memory_space=pltpu.VMEM)


def rounds(count, first):
    if count == 4 and first:
        return ((1, 3, 0, 2), (3, 2, 1, 0), (2, 0, 3, 1))
    return [[(i + step) % count for i in range(count)] for step in reversed(range(1, count))]


def everyones(value, axis, first):
    count = lax.axis_size(axis)
    if count > 8:
        copies = jnp.broadcast_to(value[None], (count,) + value.shape)
        got = lax.all_to_all(copies, axis, 0, 0, tiled=True)
        return [got[k] for k in range(count)]
    got = [value]
    for pairs in rounds(count, first):
        got.append(lax.ppermute(value, axis, list(enumerate(pairs))))
    return got


def rounded(value):
    return value.astype(BF).astype(F32)


def flat_row(ref, first, count):
    return jnp.concatenate([ref[first + i : first + i + 1, :] for i in range(count)], axis=1)


def project_kernel(tokens, other, gain, w_query, w_key, w_value, out):
    first = lax.axis_index("tp") == 0
    own = tokens[...].astype(F32)
    their = other[...].astype(F32)
    slab = jnp.concatenate([jnp.where(first, own, their), jnp.where(first, their, own)], axis=1)
    gains = flat_row(gain[...].astype(F32), 0, gain.shape[0])
    scaled = (slab * gains).astype(BF)
    q = w_query.shape[1]
    k = q + w_key.shape[1]
    v = k + w_value.shape[1]
    out[:, :q] = jnp.dot(scaled, w_query[...], preferred_element_type=F32)
    out[:, q:k] = jnp.dot(scaled, w_key[...], preferred_element_type=F32)
    out[:, k:v] = jnp.dot(scaled, w_value[...], preferred_element_type=F32)
    square = jnp.sum(slab * slab, axis=1, keepdims=True)
    out[:, v:] = jnp.broadcast_to(square, (slab.shape[0], LANES))


def attend_kernel(heads, parts, table, keys, values, out, turn):
    total = parts[0][...]
    for part in parts[1:]:
        total = total + part[...]
    rows = total.shape[0]
    span = 2 * heads
    width = total.shape[1] - LANES
    inverse = lax.rsqrt(total[:, width : width + 1] / D + EPS)
    cosine = table[0:1, :]
    sine = table[1:2, :]
    lane = lax.broadcasted_iota(jnp.int32, (rows, LANES), 1)
    near = lax.rem(lane, HD) < HD // 2

    def rotate(piece):
        ahead = pltpu.roll(piece, LANES - HD // 2, 1)
        behind = pltpu.roll(piece, HD // 2, 1)
        return rounded(piece * cosine + jnp.where(near, ahead, behind) * sine)

    pieces = [total[:, h * LANES : (h + 1) * LANES] * inverse for h in range(heads + 2)]
    for h in range(heads):
        turn[h * rows : (h + 1) * rows, :] = rotate(pieces[h]) * (HD**-0.5)
    new_key = rotate(pieces[heads])
    new_value = rounded(pieces[heads + 1])
    holds_new = lax.axis_index("kv") == 0
    lane_h = lax.broadcasted_iota(jnp.int32, (heads, LANES), 1)
    lane_s = lax.broadcasted_iota(jnp.int32, (span, LANES), 1)
    wide = []
    for r in range(rows):
        mine = turn[pl.ds(r, heads, stride=rows), :]
        wide.append(
            jnp.concatenate(
                [jnp.where(lane_h < HD, mine, 0.0), jnp.where(lane_h < HD, 0.0, mine)], axis=0
            )
        )
    scores = [
        lax.dot_general(
            wide[r].astype(BF), keys[r], (((1,), (1,)), ((), ())), preferred_element_type=F32
        )
        for r in range(rows)
    ]
    own = [
        jnp.where(holds_new, jnp.sum(wide[r] * new_key[r : r + 1, :], axis=1, keepdims=True), FAR)
        for r in range(rows)
    ]
    top = [
        jnp.maximum(jnp.max(scores[r], axis=1, keepdims=True), own[r]) for r in range(rows)
    ]
    weights = [jnp.exp(scores[r] - top[r]) for r in range(rows)]
    own_weight = [jnp.exp(own[r] - top[r]) for r in range(rows)]
    num = [
        jnp.dot(weights[r].astype(BF), values[r], preferred_element_type=F32)
        for r in range(rows)
    ]
    den = [
        jnp.sum(weights[r], axis=1, keepdims=True) + own_weight[r] for r in range(rows)
    ]
    flat = jnp.zeros((span, LANES), F32)
    for r in range(rows):
        flat = jnp.where(lane_s == r, top[r], flat)
        flat = jnp.where(lane_s == rows + r, den[r], flat)
    high = rounded(flat)
    middle = rounded(flat - high)
    low = rounded(flat - high - middle)
    stats = high + pltpu.roll(middle, 2 * rows, 1) + pltpu.roll(low, 4 * rows, 1)
    out[span * rows :, :] = stats.astype(BF)
    for r in range(rows):
        value = num[r] + rounded(own_weight[r]) * new_value[r : r + 1, :]
        out[span * r : span * (r + 1), :] = value.astype(BF)


def merge_kernel(heads, rows, messages, lam, head_gain, w_out, mine, theirs, turn):
    first = lax.axis_index("tp") == 0
    span = 2 * heads
    joined = []
    for message in messages:
        stats = message[span * rows :, :].astype(F32)
        middle = pltpu.roll(stats, LANES - 2 * rows, 1)
        low = pltpu.roll(stats, LANES - 4 * rows, 1)
        joined.append(stats + (middle + low))
    top = functools.reduce(jnp.maximum, joined)
    carried = [jnp.exp(part - top) for part in joined]
    den = sum(c * pltpu.roll(part, LANES - rows, 1) for c, part in zip(carried, joined))
    shares = [c / den for c in carried]
    sub = lax.broadcasted_iota(jnp.int32, (heads, heads), 0)
    across = lax.broadcasted_iota(jnp.int32, (heads, heads), 1)
    lams = jnp.sum(jnp.where(sub == across, lam[...], 0.0), axis=1, keepdims=True)
    gains = head_gain[...].astype(F32) * OUT_SCALE
    mixes = []
    for r in range(rows):
        ratio = sum(
            share[:, r : r + 1] * message[span * r : span * (r + 1), :].astype(F32)
            for share, message in zip(shares, messages)
        )
        mixes.append(ratio[:heads] - lams * ratio[heads:])
    means = [jnp.mean(mix * mix, axis=1, keepdims=True) for mix in mixes]
    for r in range(rows):
        turn[r * heads : (r + 1) * heads, :] = mixes[r] * lax.rsqrt(means[r] + EPS) * gains
    wide = jnp.concatenate(
        [turn[pl.ds(h, rows, stride=heads), :] for h in range(heads)], axis=1
    )
    branch = jnp.dot(wide.astype(BF), w_out[...], preferred_element_type=F32)
    half = branch.shape[1] // 2
    mine[...] = jnp.where(first, branch[:, :half], branch[:, half:]).astype(BF)
    theirs[...] = jnp.where(first, branch[:, half:], branch[:, :half]).astype(BF)


def hidden_kernel(tokens, mine, received, copies, hidden):
    branch = mine[...].astype(F32) + received[...].astype(F32)
    value = (tokens[...].astype(F32) + branch).astype(BF)
    hidden[...] = value
    for k in range(copies.shape[0]):
        copies[k] = value


def mixer_kernel(dps, everyone, gain, w_up, w_down, out):
    devices, rows, width = everyone.shape
    blocks = devices // dps
    per = width // LANES
    places = [(b % 2 * (blocks // 2) + b // 2) * dps for b in range(blocks)]
    gains = gain[...].astype(F32)
    square = jnp.zeros((dps * rows, width), F32)
    upward = jnp.zeros((dps * rows, w_up.shape[1]), F32)
    for b in range(blocks):
        block = jnp.concatenate(
            [everyone[places[b] + a].astype(F32) for a in range(dps)], axis=0
        )
        square = square + block * block
        scaled = (block * flat_row(gains, b * per, per)).astype(BF)
        upward = upward + jnp.dot(
            scaled, w_up[b * width : (b + 1) * width, :], preferred_element_type=F32
        )
    inverse = lax.rsqrt(jnp.sum(square, axis=1, keepdims=True) / D + EPS)
    act = jnp.square(jnp.maximum(upward * inverse, 0.0)).astype(BF)
    for b in range(blocks):
        down = jnp.dot(
            act, w_down[:, b * width : (b + 1) * width], preferred_element_type=F32
        ).astype(BF)
        for a in range(dps):
            out[places[b] + a] = down[a * rows : (a + 1) * rows, :]


def final_kernel(terms, hidden, out):
    total = terms[0].astype(F32)
    for k in range(1, terms.shape[0]):
        total = total + terms[k].astype(F32)
    out[...] = (hidden[...].astype(F32) + total).astype(BF)


def load_kernel(count, *refs):
    sources, held, sems = refs[:count], refs[count : 2 * count], refs[2 * count]
    copies = [
        pltpu.make_async_copy(source, target, sems.at[i])
        for i, (source, target) in enumerate(zip(sources, held))
    ]
    for copy in copies:
        copy.start()
    for copy in copies:
        copy.wait()


def loaded(*arrays):
    count = len(arrays)
    return pl.pallas_call(
        functools.partial(load_kernel, count),
        out_shape=[jax.ShapeDtypeStruct(array.shape, array.dtype) for array in arrays],
        in_specs=[pl.BlockSpec(memory_space=pltpu.HBM)] * count,
        out_specs=[VMEM] * count,
        scratch_shapes=[pltpu.SemaphoreType.DMA((count,))],
        compiler_params=pltpu.CompilerParams(vmem_limit_bytes=1 << 20),
        cost_estimate=pl.CostEstimate(
            flops=8 << 30, bytes_accessed=8 << 20, transcendentals=0
        ),
    )(*(pltpu.with_memory_space_constraint(array, pltpu.HBM) for array in arrays))


def tables(position):
    half = HD // 2
    angle = position * THETA ** (-np.arange(half, dtype=np.float64) * 2.0 / HD)
    cosine = np.tile(np.cos(angle), LANES // half)
    sine = np.tile(np.concatenate([-np.sin(angle), np.sin(angle)]), LANES // HD)
    rest = np.zeros((6, LANES))
    return jnp.asarray(np.concatenate([cosine[None], sine[None], rest]), F32)


def call(kernel, shapes, inputs, mib, cost=1, scratch=()):
    return pl.pallas_call(
        kernel,
        out_shape=shapes,
        in_specs=[VMEM] * len(inputs),
        out_specs=jax.tree.map(lambda _: VMEM, shapes),
        scratch_shapes=[pltpu.VMEM(shape, F32) for shape in scratch],
        compiler_params=pltpu.CompilerParams(vmem_limit_bytes=mib << 20),
        cost_estimate=pl.CostEstimate(
            flops=cost << 30, bytes_accessed=cost << 20, transcendentals=0
        ),
    )(*inputs)


def local(
    tokens,
    attn_gain,
    w_query,
    w_key,
    w_value,
    key_cache,
    value_cache,
    lam,
    head_gain,
    w_out,
    ffn_gain,
    w_up,
    w_down,
):
    rows, width = tokens.shape
    kv_count = lax.axis_size("kv")
    tp_count = lax.axis_size("tp")
    dp_count = lax.axis_size("dp")
    positions = key_cache.shape[1]
    heads = lam.shape[0]
    axes = ("tp", "kv", "dp")
    swap = [(0, 1), (1, 0)]
    assert tp_count == 2 and key_cache.shape[2] == 1 and 6 * rows <= LANES
    shape = jax.ShapeDtypeStruct

    other = lax.ppermute(tokens, "tp", swap)
    packed = w_query.shape[1] + w_key.shape[1] + w_value.shape[1] + LANES
    held, gain = loaded(tokens, attn_gain.reshape(-1, LANES))
    part = call(
        project_kernel,
        shape((rows, packed), F32),
        (held, other, gain, w_query, w_key, w_value),
        6,
        8,
    )
    parts = everyones(part, "kv", True)
    count = len(parts)

    def attend(*refs):
        attend_kernel(heads, refs[:count], *refs[count:])

    message = call(
        attend,
        shape((2 * heads * (rows + 1), LANES), BF),
        (
            *parts,
            tables(positions * kv_count),
            key_cache.reshape(rows, positions, 2 * HD),
            value_cache.reshape(rows, positions, VD),
        ),
        8,
        8,
        [(heads * rows, LANES)],
    )
    messages = everyones(message, "kv", False)

    def merge(*refs):
        merge_kernel(heads, rows, refs[:count], *refs[count:])

    mine, theirs = call(
        merge,
        (shape((rows, width), BF), shape((rows, width), BF)),
        (*messages, lam.reshape(1, heads), head_gain.reshape(1, VD), w_out),
        5,
        8,
        [(heads * rows, LANES)],
    )
    received = lax.ppermute(theirs, "tp", swap)
    devices = dp_count * kv_count * tp_count
    copies, hidden = call(
        hidden_kernel,
        (shape((devices, rows, width), BF), shape((rows, width), BF)),
        (held, mine, received),
        2,
    )
    everyone = lax.all_to_all(copies, axes, 0, 0, tiled=True)
    term = call(
        functools.partial(mixer_kernel, dp_count),
        shape((devices, rows, width), BF),
        (everyone, ffn_gain.reshape(-1, LANES), w_up, w_down),
        12,
    )
    terms = lax.all_to_all(term, axes, 0, 0, tiled=True)
    return call(final_kernel, shape((rows, width), BF), (terms, hidden), 2)


def solution(mesh):
    in_specs = (
        P("dp", ("kv", "tp")),
        P("kv"),
        P("kv", "tp"),
        P("kv", "tp"),
        P("kv", "tp"),
        P("dp", "kv", "tp", None),
        P("dp", "kv", "tp", None),
        P("tp"),
        P(),
        P("tp", "kv"),
        P(),
        P(None, ("dp", "kv", "tp")),
        P(("dp", "kv", "tp"), None),
    )
    out_specs = P("dp", ("kv", "tp"))
    return jax.shard_map(local, mesh=mesh, in_specs=in_specs, out_specs=out_specs, check_vma=False)
```
